32 devices in a mesh: grp: 2 (over y), sp: 16 (over z, x, core), tp: 1.
Axes of the slice: x: 2, y: 2, z: 4, core: 2. Of those that a mesh axis runs over, the one named last changes fastest.
Arguments:
- resid: bfloat16 [8192, 2048], P(('grp', 'sp', 'tp')), parts along dimension 0, may hold values from -6 to 6
- gate_b: bfloat16 [8192, 2048], P(('grp', 'sp'), 'tp'), parts along dimension 0, may hold values from -6 to 6
- gate_c: bfloat16 [8192, 2048], P(('grp', 'sp'), 'tp'), parts along dimension 0, may hold values from -6 to 6
- value: bfloat16 [8192, 2048], P(('grp', 'sp'), 'tp'), parts along dimension 0, may hold values from -6 to 6
- taps: bfloat16 [3, 2048], P(None, 'tp'), may hold values from -3.5 to 3.5
- doc_ids: int32 [8192], P(('grp', 'sp')), parts along dimension 0, may hold values from 0 to 3, never falling along the last dimension, each value on 1 to 2048 neighbouring positions
- out_weight: bfloat16 [2048, 2048], P('tp'), may hold values from -0.125 to 0.125
- norm_gains: float32 [3, 2048], replicated, may hold values from 0.1 to 1.9
- routes: int32 [8192, 2], P(('grp', 'sp')), parts along dimension 0, may hold values from 0 to 15, all different within a row; in each aligned block of 256 rows (0 to 255, 256 to 511, ...) at most 48 rows name the same one
- route_weights: float32 [8192, 2], P(('grp', 'sp')), parts along dimension 0, may hold values from 0.2 to 1
- w_gate: bfloat16 [16, 2048, 4096], P('sp', None, 'tp'), may hold values from -0.125 to 0.125
- w_up: bfloat16 [16, 2048, 4096], P('sp', None, 'tp'), may hold values from -0.125 to 0.125
- w_down: bfloat16 [16, 4096, 2048], P('sp', 'tp'), may hold values from -0.09375 to 0.09375
Outputs:
- layer_out: bfloat16 [8192, 2048], P(('grp', 'sp', 'tp')), parts along dimension 0
The draws below stay inside these ranges and needn't reach their ends.
There are 2 independent parts, one for each index of `grp`. The reference program is written for one: setup_inputs(seed, part) draws one part's arguments, and reference() takes and returns one part's arrays. A program takes and returns all parts, laid end to end along the dimension named above; an argument that names none is the same for every part. Nothing has to cross between parts.
Inputs may be any that keep to these rules, and one draw needn't show every extreme that they name: `doc_ids`: never falling along the sequence; each document spans 1 to 2048 positions. `routes`: each row names 2 different experts. In each aligned block of 256 rows no expert is named more than 48 times, and in every draw some block names some expert exactly 48 times.
All inputs are finite; a program needn't handle non-finite values.
Results may differ from the reference program's by a relative error of at most 0.02.
Values may be sent and summed in bfloat16 or wider, within the bound.
No kernel may reach another device: no remote copies, remote signals or barrier semaphores. Data moves between devices by JAX's collectives and lax.ppermute only.
A program may use at most 128 MiB of HBM per device.

```python
import math
import jax
import jax.numpy as jnp
import numpy as np
from jax import lax

D = 2048
FF = 4096
TAPS = 3
TOP = 2
TOKENS = 4096
ROWS_BLK = 256
EXPERTS = 16
CAP = 48
DOCS = 4
DOC_MOST = 2048
N_TP = 1


def steps_of(key, dims, cuts, least, high):
    loudness, own = 1.0, jax.random.fold_in(key, 6)
    for position, shards_of in cuts:
        steps = jnp.exp(jax.random.uniform(jax.random.fold_in(own, position), (shards_of,), jnp.float32, least / len(cuts), high / len(cuts)))
        loudness = loudness * jnp.repeat(steps, dims[position] // shards_of).reshape([-1 if axis == position else 1 for axis in range(len(dims))])
    return loudness


def profile(amount, total, most, lean):
    weights = [(1 << 20) // math.isqrt(rank ** lean) + 1 for rank in range(2, amount + 1)]
    rest, counts = total - most - (amount - 1), [1] * (amount - 1)
    while rest > 0:
        movable = [i for i in range(amount - 1) if counts[i] < most]
        whole, budget = sum([weights[i] for i in movable]), rest
        for i in movable:
            more = min(most - counts[i], max(1, budget * weights[i] // whole), rest)
            counts[i] = counts[i] + more
            rest = rest - more
    return np.array([most] + counts)


def uneven(rng, amount, total, reach, slope):
    if amount == 2:
        one = jax.random.randint(rng, (), max(1, total - reach), min(reach, total - 1) + 1)
        return jnp.stack([one, total - one])
    sizes = jnp.asarray(profile(amount, total, reach, slope), jnp.int32)
    twos = (amount - 1) // 2
    source_of, receiver = sizes[1:1 + 2 * twos:2], sizes[2:2 + 2 * twos:2]
    margin = jnp.minimum(source_of - 1, reach - receiver)
    shifted = jax.random.randint(jax.random.fold_in(rng, 1), (twos,), 0, 1 << 20) % (margin + 1)
    sizes = sizes.at[1:1 + 2 * twos:2].set(source_of - shifted).at[2:2 + 2 * twos:2].set(receiver + shifted)
    return sizes[jax.random.permutation(jax.random.fold_in(rng, 2), amount)]


def shared_out(rng, own, number, rows, amount, top, limit, lean):
    sequence = jax.random.permutation(rng, amount)
    packed, common = load_shares(amount, rows * top, limit, lean, True), load_shares(amount, rows * top, limit, lean, False)
    places = jnp.arange(amount)

    def named(lengths, offset_by):
        used = int((lengths > 0).sum())
        fixed = max(1, used // 4)
        shifted = fixed + (places - fixed + offset_by * (used - fixed)) % max(1, amount - fixed)
        return jnp.zeros((amount,), jnp.int32).at[sequence[jnp.where(places < fixed, places, shifted)]].set(jnp.asarray(lengths, jnp.int32))

    lengths = jnp.where(number % 4 == 0, named(packed, number // 4), named(common, number - number // 4 - 1))
    mixed = jax.random.permutation(jax.random.fold_in(own, 3), amount)
    giver, receiver = mixed[0:amount // 2 * 2:2], mixed[1:amount // 2 * 2:2]
    slack = jnp.minimum(lengths[giver] - 1, limit - lengths[receiver]) // 2
    slack = jnp.where((giver == sequence[0]) | (receiver == sequence[0]) | (lengths[receiver] == 0), 0, jnp.maximum(slack, 0))
    shifted = jax.random.randint(jax.random.fold_in(own, 4), (amount // 2,), 0, 1 << 20) % (slack + 1)
    lengths = lengths.at[giver].add(-shifted).at[receiver].add(shifted)
    members = jnp.searchsorted(jnp.cumsum(lengths), jnp.arange(rows * top), side="right").astype(jnp.int32)
    listing = members.reshape(top, rows).T
    listing = listing[jax.random.permutation(jax.random.fold_in(own, 1), rows)]
    offset_by = jax.random.randint(jax.random.fold_in(own, 2), (rows, 1), 0, top)
    return jnp.take_along_axis(listing, (jnp.arange(top)[None, :] + offset_by) % top, axis=1)


def load_shares(amount, total, most, skew, full):
    portions = [(1 << 20) // math.isqrt(standing ** skew) + 1 for standing in range(1, amount + 1)]
    largest = most if full else min(most, max(-(-total // amount), total * portions[0] // sum(portions)))
    least = 1 if total - largest >= amount - 1 else 0
    holding, spare = [largest] + [least] * (amount - 1), total - largest - least * (amount - 1)
    while spare > 0:
        free = [i for i in range(1, amount) if holding[i] < largest] or [i for i in range(1, amount) if holding[i] < most]
        mass, remaining = sum([portions[i] for i in free]), spare
        for i in free:
            extra = min(most - holding[i], max(1, remaining * portions[i] // mass), spare)
            holding[i] = holding[i] + extra
            spare = spare - extra
    return np.array(holding)


def bell_draw(rng, shape, deviation, limit, pieces=(), held_as=jnp.bfloat16):
    values = deviation * jax.random.normal(rng, shape, jnp.float32)
    if pieces:
        values = values * steps_of(rng, shape, pieces, -0.22, 0.18)
    return jnp.clip(values, -limit, limit).astype(held_as)


def setup_inputs(seed: int = 0, part: int = 0) -> dict:
    key_of = jax.random.split(jax.random.key(seed), 14)
    own_keys = jax.random.split(jax.random.fold_in(key_of[13], part), 14)
    resid = bell_draw(own_keys[0], (TOKENS, D), 1.0, 6.0, ((0, 16),))
    gate_b = bell_draw(own_keys[1], (TOKENS, D), 1.0, 6.0, ((0, 16),))
    gate_c = bell_draw(own_keys[2], (TOKENS, D), 1.0, 6.0, ((0, 16),))
    value = bell_draw(own_keys[3], (TOKENS, D), 1.0, 6.0, ((0, 16),))
    taps = bell_draw(key_of[4], (TAPS, D), TAPS ** -0.5, 3.5)
    doc_ids = jnp.searchsorted(jnp.cumsum(uneven(own_keys[5], DOCS, TOKENS, DOC_MOST, 1)), jnp.arange(TOKENS), side="right").astype(jnp.int32)
    out_weight = bell_draw(key_of[6], (D, D), D ** -0.5, 0.125)
    norm_gains = jnp.clip(1.0 + 0.18 * jax.random.normal(key_of[7], (3, D), jnp.float32), 0.1, 1.9)
    routes_keys = jax.random.split(jax.random.fold_in(own_keys[8], 1), TOKENS // ROWS_BLK)
    routes_turns = jax.random.permutation(jax.random.fold_in(own_keys[8], 3), TOKENS // ROWS_BLK)
    routes = jax.vmap(lambda own, number: shared_out(jax.random.fold_in(own_keys[8], 2), own, number, ROWS_BLK, EXPERTS, TOP, CAP, 1))(routes_keys, routes_turns).reshape((TOKENS, TOP))
    route_weights = jnp.clip(0.2 + 0.8 * jax.random.uniform(own_keys[9], (TOKENS, TOP), jnp.float32) ** steps_of(own_keys[9], (TOKENS, TOP), ((0, 16),), -0.2, 0.2), 0.2, 1.0)
    w_gate = bell_draw(key_of[10], (EXPERTS, D, FF), D ** -0.5, 0.125, ((0, 16),))
    w_up = bell_draw(key_of[11], (EXPERTS, D, FF), D ** -0.5, 0.125, ((0, 16),))
    w_down = bell_draw(key_of[12], (EXPERTS, FF, D), FF ** -0.5, 0.09375, ((0, 16),))
    return {"resid": resid, "gate_b": gate_b, "gate_c": gate_c, "value": value, "taps": taps, "doc_ids": doc_ids, "out_weight": out_weight, "norm_gains": norm_gains, "routes": routes, "route_weights": route_weights, "w_gate": w_gate, "w_up": w_up, "w_down": w_down}


norm_eps = 1e-06

def rms_scale(values, gain_row):
    mean_sq = lax.optimization_barrier(jnp.mean(values * values, axis=-1, keepdims=True))
    return values * lax.rsqrt(mean_sq + norm_eps) * gain_row

def slot_table(block_routes, experts, capacity):
    block_count = block_routes.shape[0]
    block_len = block_routes.shape[1]
    flat_routes = block_routes.reshape(block_count, block_len * TOP)
    onehot = (flat_routes[:, :, None] == jnp.arange(experts, dtype=jnp.int32)[None, None, :]).astype(jnp.int32)
    before = (jnp.cumsum(onehot, axis=1) - onehot).astype(jnp.int32)
    slot_rank = lax.optimization_barrier(jnp.sum(before * onehot, axis=2)).astype(jnp.int32)
    slot_hit = onehot[:, :, :, None] * (slot_rank[:, :, None, None] == jnp.arange(capacity, dtype=jnp.int32)[None, None, None, :]).astype(jnp.int32)
    owner_row = jnp.arange(block_len * TOP, dtype=jnp.int32) // TOP
    slot_tok = lax.optimization_barrier(jnp.sum(slot_hit * owner_row[None, :, None, None], axis=1)).astype(jnp.int32)
    filled = lax.optimization_barrier(jnp.sum(slot_hit, axis=1)).astype(jnp.int32)
    return (slot_rank.reshape(block_count, block_len, TOP), slot_tok, filled)

def grouped_product(left_rows, right_rows, groups):
    group_width = left_rows.shape[1] // groups

    def add_group(running, group_index):
        first = group_index * group_width
        block_cols = lax.dynamic_slice_in_dim(left_rows, first, group_width, 1)
        block_rows = lax.dynamic_slice_in_dim(right_rows, first, group_width, 0)
        group_term = jnp.dot(block_cols, block_rows, preferred_element_type=jnp.float32).astype(jnp.bfloat16)
        group_term = lax.optimization_barrier(group_term)
        return (running + group_term.astype(jnp.float32), None)
    start_sum = jnp.zeros((left_rows.shape[0], right_rows.shape[1]), jnp.float32)
    running, _ = lax.scan(add_group, start_sum, jnp.arange(groups, dtype=jnp.int32))
    return running

def reference(resid, gate_b, gate_c, value, taps, doc_ids, out_weight, norm_gains, routes, route_weights, w_gate, w_up, w_down):
    product = gate_c.astype(jnp.float32) * value.astype(jnp.float32)
    tap_weights = taps.astype(jnp.float32)
    convolved = tap_weights[0] * product
    for distance in range(1, TAPS):
        earlier = jnp.pad(product, ((distance, 0), (0, 0)))[:TOKENS]
        earlier_ids = jnp.pad(doc_ids, (distance, 0), constant_values=-1)[:TOKENS]
        same_doc = earlier_ids == doc_ids
        convolved = convolved + jnp.where(same_doc[:, None], tap_weights[distance] * earlier, 0.0)
    mixed_rows = (gate_b.astype(jnp.float32) * convolved).astype(jnp.bfloat16)
    projected = grouped_product(mixed_rows, out_weight, N_TP)
    gain_rows = norm_gains.astype(jnp.float32)
    stream = resid.astype(jnp.float32) + rms_scale(projected, gain_rows[0])
    normed = rms_scale(stream, gain_rows[1]).astype(jnp.bfloat16)
    blocks = TOKENS // ROWS_BLK
    slot_rank, slot_tok, filled = slot_table(routes.reshape(blocks, ROWS_BLK, TOP), EXPERTS, CAP)
    normed_blocks = normed.reshape(blocks, ROWS_BLK, D)

    def one_expert(expert):
        slot_picks = slot_tok[:, expert]
        slot_live = filled[:, expert]
        picked_rows = jax.vmap(lambda block_rows, picks: block_rows[picks])(normed_blocks, slot_picks)
        picked_rows = jnp.where(slot_live[:, :, None] > 0, picked_rows, jnp.zeros_like(picked_rows))
        picked_rows = picked_rows.reshape(blocks * CAP, D)
        gate_proj = jnp.dot(picked_rows, w_gate[expert], preferred_element_type=jnp.float32)
        up_proj = jnp.dot(picked_rows, w_up[expert], preferred_element_type=jnp.float32)
        hidden = (jax.nn.silu(gate_proj) * up_proj).astype(jnp.bfloat16)
        expert_out = grouped_product(hidden, w_down[expert], N_TP).astype(jnp.bfloat16)
        return expert_out.reshape(blocks, CAP, D)
    expert_out = lax.map(one_expert, jnp.arange(EXPERTS, dtype=jnp.int32))
    block_index = jnp.arange(TOKENS, dtype=jnp.int32) // ROWS_BLK
    picked = expert_out[routes, block_index[:, None], slot_rank.reshape(TOKENS, TOP)]
    shares = route_weights / lax.optimization_barrier(jnp.sum(route_weights, axis=1, keepdims=True))
    combined = lax.optimization_barrier(jnp.sum(shares[:, :, None] * picked.astype(jnp.float32), axis=1))
    return (stream + rms_scale(combined, gain_rows[2])).astype(jnp.bfloat16)
```

```python
import math

import jax
import jax.numpy as jnp
from jax import lax
from jax.experimental import pallas as pl
from jax.experimental.pallas import tpu as pltpu
from jax.sharding import PartitionSpec as P


TAPS = 3
TOP = 2
CHUNKS = 2

norm_eps = 1e-06


def passed_along(block, axis, distance):
    devices = range(lax.axis_size(axis))
    route = [(i - distance, i) for i in devices if i - distance in devices]
    return lax.ppermute(block, axis, route)


def rms_scale(values, gain_row):
    mean_sq = jnp.mean(values * values, axis=-1, keepdims=True)
    return values * lax.rsqrt(mean_sq + norm_eps) * gain_row


def dot_f32(a, b, dims):
    return lax.dot_general(a, b, (dims, ((), ())), preferred_element_type=jnp.float32)


def route_tables(my_routes, my_weights, experts):
    rows = my_routes.shape[0]
    expert_ids = lax.broadcasted_iota(jnp.int32, (rows, experts), 1)
    shares = my_weights / jnp.sum(my_weights, axis=1, keepdims=True)
    named = jnp.zeros((rows, experts), jnp.bool_)
    share_of = jnp.zeros((rows, experts), jnp.float32)
    for k in range(TOP):
        hit = my_routes[:, k : k + 1] == expert_ids
        named = named | hit
        share_of = share_of + jnp.where(hit, shares[:, k : k + 1], 0.0)
    earlier = (
        lax.broadcasted_iota(jnp.int32, (rows, rows), 0)
        > lax.broadcasted_iota(jnp.int32, (rows, rows), 1)
    ).astype(jnp.bfloat16)
    before = dot_f32(earlier, named.astype(jnp.bfloat16), ((1,), (0,)))
    slot_of = jnp.where(named, before, -1.0).astype(jnp.bfloat16)
    high = lax.reduce_precision(share_of, 8, 7)
    return slot_of, high.astype(jnp.bfloat16), (share_of - high).astype(jnp.bfloat16)


def chunk_tables(tables, experts, first, size):
    slot_of, high, low = tables
    cols = lax.broadcasted_iota(jnp.int32, (experts, experts * size), 1)
    owner = lax.broadcasted_iota(jnp.int32, (experts, experts * size), 0)
    spread = (cols // size == owner).astype(jnp.bfloat16)
    col_slot = (lax.broadcasted_iota(jnp.int32, (1, experts * size), 1) % size + first).astype(jnp.float32)
    taken = dot_f32(slot_of, spread, ((1,), (0,))) == col_slot
    onehot = taken.astype(jnp.bfloat16)
    w_high = jnp.where(taken, dot_f32(high, spread, ((1,), (0,))), 0.0).astype(jnp.bfloat16)
    w_low = jnp.where(taken, dot_f32(low, spread, ((1,), (0,))), 0.0).astype(jnp.bfloat16)
    return onehot, w_high, w_low


def expert_body(rows_ref, gate_ref, up_ref, down_ref, out_ref, acc_ref):
    step = pl.program_id(0)
    rows = rows_ref[...]
    gate_proj = jnp.dot(rows, gate_ref[0], preferred_element_type=jnp.float32)
    up_proj = jnp.dot(rows, up_ref[0], preferred_element_type=jnp.float32)
    hidden = (gate_proj / (1.0 + jnp.exp(-gate_proj)) * up_proj).astype(jnp.bfloat16)
    part = jnp.dot(hidden, down_ref[0], preferred_element_type=jnp.float32)

    @pl.when(step == 0)
    def _():
        acc_ref[...] = part

    @pl.when(step > 0)
    def _():
        acc_ref[...] += part

    @pl.when(step == pl.num_programs(0) - 1)
    def _():
        out_ref[...] = acc_ref[...].astype(out_ref.dtype)


def expert_block(rows, w_gate, w_up, w_down):
    count, width = rows.shape
    units = w_gate.shape[2]
    block = math.gcd(units, 512)
    return pl.pallas_call(
        expert_body,
        grid=(units // block,),
        in_specs=[
            pl.BlockSpec((count, width), lambda j: (0, 0)),
            pl.BlockSpec((1, width, block), lambda j: (0, 0, j)),
            pl.BlockSpec((1, width, block), lambda j: (0, 0, j)),
            pl.BlockSpec((1, block, width), lambda j: (0, j, 0)),
        ],
        out_specs=pl.BlockSpec((count, width), lambda j: (0, 0)),
        out_shape=jax.ShapeDtypeStruct((count, width), jnp.bfloat16),
        scratch_shapes=[pltpu.VMEM((count, width), jnp.float32)],
        cost_estimate=pl.CostEstimate(
            flops=6 * count * width * units,
            transcendentals=count * units,
            bytes_accessed=6 * width * units + 4 * count * width,
        ),
        compiler_params=pltpu.CompilerParams(
            dimension_semantics=("arbitrary",), vmem_limit_bytes=48 * 2**20
        ),
        name="experts",
    )(rows, w_gate, w_up, w_down)


def mixer_rows(gate_b, gate_c, value, taps, doc_ids):
    tok_dev, width = gate_b.shape
    tap_reach = TAPS - 1
    ids_bf = jnp.broadcast_to(doc_ids[tok_dev - tap_reach :, None], (tap_reach, 128)).astype(jnp.bfloat16)
    packed = jnp.concatenate([gate_c[tok_dev - tap_reach :], value[tok_dev - tap_reach :], ids_bf], axis=1)
    got = passed_along(packed, "sp", 1).astype(jnp.float32)
    prev_rows = got[:, :width] * got[:, width : 2 * width]
    id_values = doc_ids.astype(jnp.float32)
    ext_ids = jnp.concatenate([got[:, 2 * width], id_values], axis=0)
    product = gate_c.astype(jnp.float32) * value.astype(jnp.float32)
    ext_rows = jnp.concatenate([prev_rows, product], axis=0)
    tap_weights = taps.astype(jnp.float32)
    convolved = tap_weights[0] * product
    for distance in range(1, TAPS):
        earlier = ext_rows[tap_reach - distance : tap_reach - distance + tok_dev]
        same_doc = ext_ids[tap_reach - distance : tap_reach - distance + tok_dev] == id_values
        convolved = convolved + jnp.where(same_doc[:, None], tap_weights[distance] * earlier, 0.0)
    return (gate_b.astype(jnp.float32) * convolved).astype(jnp.bfloat16)


def per_device(
    resid,
    gate_b,
    gate_c,
    value,
    taps,
    doc_ids,
    out_weight,
    norm_gains,
    routes,
    route_weights,
    w_gate,
    w_up,
    w_down,
):
    rows_blk = resid.shape[0]
    width = resid.shape[1]
    experts = lax.axis_size("sp")
    capacity = max(2, 3 * TOP * rows_blk // (2 * experts))
    offset = lax.axis_index("tp") * rows_blk
    my_routes = lax.dynamic_slice_in_dim(routes, offset, rows_blk, 0)
    my_weights = lax.dynamic_slice_in_dim(route_weights, offset, rows_blk, 0)
    tables = route_tables(my_routes, my_weights, experts)
    edges = [capacity * c // CHUNKS for c in range(CHUNKS + 1)]
    chunks = [chunk_tables(tables, experts, a, b - a) for a, b in zip(edges, edges[1:])]

    mixed = mixer_rows(gate_b, gate_c, value, taps, doc_ids)
    projected = lax.psum_scatter(
        jnp.dot(mixed, out_weight, preferred_element_type=jnp.float32).astype(jnp.bfloat16),
        "tp",
        scatter_dimension=0,
        tiled=True,
    ).astype(jnp.float32)
    stream = resid.astype(jnp.float32) + rms_scale(projected, norm_gains[0])
    normed = rms_scale(stream, norm_gains[1]).astype(jnp.bfloat16)

    combined = 0.0
    for (onehot, w_high, w_low), first, last in zip(chunks, edges, edges[1:]):
        size = last - first
        outgoing = dot_f32(onehot, normed, ((0,), (0,))).astype(jnp.bfloat16)
        arrived = lax.all_to_all(outgoing.reshape(experts, size, width), "sp", split_axis=0, concat_axis=0, tiled=True)
        rows = lax.all_gather(arrived[None], "tp", axis=0, tiled=True).reshape(-1, width)
        worked = expert_block(rows, w_gate, w_up, w_down)
        result = lax.psum_scatter(worked, "tp", scatter_dimension=0, tiled=True).reshape(experts, size, width)
        returned = lax.all_to_all(result, "sp", split_axis=0, concat_axis=0, tiled=True).reshape(-1, width)
        combined = combined + dot_f32(w_high, returned, ((1,), (0,))) + dot_f32(w_low, returned, ((1,), (0,)))
    return (stream + rms_scale(combined, norm_gains[2])).astype(jnp.bfloat16)


def solution(mesh):
    return jax.shard_map(
        per_device,
        mesh=mesh,
        in_specs=(
            P(("grp", "sp", "tp"), None),
            P(("grp", "sp"), "tp"),
            P(("grp", "sp"), "tp"),
            P(("grp", "sp"), "tp"),
            P(None, "tp"),
            P(("grp", "sp")),
            P("tp", None),
            P(),
            P(("grp", "sp"), None),
            P(("grp", "sp"), None),
            P("sp", None, "tp"),
            P("sp", None, "tp"),
            P("sp", "tp", None),
        ),
        out_specs=P(("grp", "sp", "tp"), None),
        check_vma=False,
    )
```

```python
import functools
import math

import jax
import jax.numpy as jnp
from jax import lax
from jax.experimental import pallas as pl
from jax.experimental.pallas import tpu as pltpu
from jax.sharding import PartitionSpec as P


TAPS = 3
TOP = 2
CHUNKS = 2

norm_eps = 1e-06


def passed_along(block, axis, distance):
    devices = range(lax.axis_size(axis))
    route = [(i - distance, i) for i in devices if i - distance in devices]
    return lax.ppermute(block, axis, route)


def rms_scale(values, gain_row):
    mean_sq = jnp.mean(values * values, axis=-1, keepdims=True)
    return values * lax.rsqrt(mean_sq + norm_eps) * gain_row


def dot_f32(a, b, dims):
    return lax.dot_general(a, b, (dims, ((), ())), preferred_element_type=jnp.float32)


def route_tables(my_routes, my_weights, experts):
    rows = my_routes.shape[0]
    expert_ids = lax.broadcasted_iota(jnp.int32, (rows, experts), 1)
    shares = my_weights / jnp.sum(my_weights, axis=1, keepdims=True)
    named = jnp.zeros((rows, experts), jnp.bool_)
    share_of = jnp.zeros((rows, experts), jnp.float32)
    for k in range(TOP):
        hit = my_routes[:, k : k + 1] == expert_ids
        named = named | hit
        share_of = share_of + jnp.where(hit, shares[:, k : k + 1], 0.0)
    earlier = (
        lax.broadcasted_iota(jnp.int32, (rows, rows), 0)
        > lax.broadcasted_iota(jnp.int32, (rows, rows), 1)
    ).astype(jnp.bfloat16)
    before = dot_f32(earlier, named.astype(jnp.bfloat16), ((1,), (0,)))
    slot_of = jnp.where(named, before, -1.0).astype(jnp.bfloat16)
    high = lax.reduce_precision(share_of, 8, 7)
    return slot_of, high.astype(jnp.bfloat16), (share_of - high).astype(jnp.bfloat16)


def chunk_tables(tables, experts, first, size):
    slot_of, high, low = tables
    cols = lax.broadcasted_iota(jnp.int32, (experts, experts * size), 1)
    owner = lax.broadcasted_iota(jnp.int32, (experts, experts * size), 0)
    spread = (cols // size == owner).astype(jnp.bfloat16)
    col_slot = (lax.broadcasted_iota(jnp.int32, (1, experts * size), 1) % size + first).astype(jnp.float32)
    taken = dot_f32(slot_of, spread, ((1,), (0,))) == col_slot
    onehot = taken.astype(jnp.bfloat16)
    w_high = jnp.where(taken, dot_f32(high, spread, ((1,), (0,))), 0.0).astype(jnp.bfloat16)
    w_low = jnp.where(taken, dot_f32(low, spread, ((1,), (0,))), 0.0).astype(jnp.bfloat16)
    return onehot, w_high, w_low


def expert_block(rows, w_gate, w_up, w_down):
    return expert_blocks([rows], w_gate, w_up, w_down)[0]


def earlier_than(rows, axis):
    i = lax.broadcasted_iota(jnp.int32, (rows, rows), axis)
    j = lax.broadcasted_iota(jnp.int32, (rows, rows), 1 - axis)
    return jnp.where(i < j, 1.0, 0.0).astype(jnp.bfloat16)


def pick_body(partners, cap, routes_ref, normed_ref, *out_refs):
    rows = normed_ref.shape[0]
    ids = lax.broadcasted_iota(jnp.int32, (partners, rows), 0)
    named = jnp.zeros((partners, rows), jnp.float32)
    for k in range(TOP):
        named = named + jnp.where(routes_ref[k : k + 1, :] == ids, 1.0, 0.0)
    before = dot_f32(named.astype(jnp.bfloat16), earlier_than(rows, 0), ((1,), (0,)))
    slot_of = jnp.where(named > 0.0, before, -1.0).astype(jnp.bfloat16)
    group = math.gcd(partners, 4)
    normed = normed_ref[...]
    for first in range(0, partners, group):
        line = lax.broadcasted_iota(jnp.int32, (group * cap, partners), 0)
        start = (lax.broadcasted_iota(jnp.int32, (group * cap, partners), 1) - first) * cap
        mine = (line >= start) & (line < start + cap)
        slot = jnp.sum(jnp.where(mine, (line - start).astype(jnp.float32), 0.0), axis=1, keepdims=True)
        spread = jnp.where(mine, 1.0, 0.0).astype(jnp.bfloat16)
        taken = dot_f32(spread, slot_of, ((1,), (0,))) == slot
        onehot = jnp.where(taken, 1.0, 0.0).astype(jnp.bfloat16)
        picked = dot_f32(onehot, normed, ((1,), (0,))).astype(jnp.bfloat16)
        for b in range(group):
            out_refs[first + b][...] = picked[b * cap : (b + 1) * cap]


def pick_blocks(partner_t, normed, partners, cap):
    width = normed.shape[1]
    return pl.pallas_call(
        functools.partial(pick_body, partners, cap),
        out_shape=[jax.ShapeDtypeStruct((cap, width), jnp.bfloat16)] * partners,
        compiler_params=pltpu.CompilerParams(vmem_limit_bytes=48 * 2**20),
        name="pick",
    )(partner_t, normed)


def share_columns(partner, share, partners, first, count, cap):
    rows = partner.shape[0]
    ids = lax.broadcasted_iota(jnp.int32, (rows, partners), 1)
    total = share[:, 0:1]
    for k in range(1, TOP):
        total = total + share[:, k : k + 1]
    named = jnp.zeros((rows, partners), jnp.float32)
    share_of = jnp.zeros((rows, partners), jnp.float32)
    for k in range(TOP):
        hit = partner[:, k : k + 1] == ids
        named = named + jnp.where(hit, 1.0, 0.0)
        share_of = share_of + jnp.where(hit, share[:, k : k + 1] / total, 0.0)
    before = dot_f32(earlier_than(rows, 1), named.astype(jnp.bfloat16), ((1,), (0,)))
    slot_of = jnp.where(named > 0.0, before, -1.0).astype(jnp.bfloat16)
    high = share_of.astype(jnp.bfloat16)
    low = (share_of - high.astype(jnp.float32)).astype(jnp.bfloat16)
    cols = lax.broadcasted_iota(jnp.int32, (partners, count * cap), 1)
    start = (lax.broadcasted_iota(jnp.int32, (partners, count * cap), 0) - first) * cap
    mine = (cols >= start) & (cols < start + cap)
    slot = jnp.sum(jnp.where(mine, (cols - start).astype(jnp.float32), 0.0), axis=0, keepdims=True)
    spread = jnp.where(mine, 1.0, 0.0).astype(jnp.bfloat16)
    taken = dot_f32(slot_of, spread, ((1,), (0,))) == slot
    return [
        jnp.where(taken, dot_f32(part, spread, ((1,), (0,))), 0.0).astype(jnp.bfloat16) for part in (high, low)
    ]


def weighted_sum(partners, first, partner_ref, share_ref, block_refs, rows_ref):
    cap = block_refs[0].shape[0]
    for b, ref in enumerate(block_refs):
        rows_ref[b * cap : (b + 1) * cap, :] = ref[...]
    high, low = share_columns(partner_ref[...], share_ref[...], partners, first, len(block_refs), cap)
    rows = rows_ref[...]
    return dot_f32(high, rows, ((1,), (0,))) + dot_f32(low, rows, ((1,), (0,)))


def join_body(partners, first, partner_ref, share_ref, *refs):
    *block_refs, out_ref, rows_ref = refs
    out_ref[...] = weighted_sum(partners, first, partner_ref, share_ref, block_refs, rows_ref)


def last_body(partners, first, partner_ref, share_ref, gain_ref, stream_ref, part_ref, *refs):
    *block_refs, out_ref, rows_ref = refs
    combined = part_ref[...] + weighted_sum(partners, first, partner_ref, share_ref, block_refs, rows_ref)
    out_ref[...] = (stream_ref[...] + rms_scale(combined, gain_ref[...])).astype(out_ref.dtype)


def join_call(body, partners, first, given, blocks, out):
    cap, width = blocks[0].shape
    return pl.pallas_call(
        functools.partial(body, partners, first),
        out_shape=out,
        scratch_shapes=[pltpu.VMEM((len(blocks) * cap, width), jnp.bfloat16)],
        compiler_params=pltpu.CompilerParams(vmem_limit_bytes=48 * 2**20),
        name="join",
    )(*given, *blocks)


def expert_body(count, *refs):
    in_refs, (gate_ref, up_ref, down_ref) = refs[:count], refs[count : count + 3]
    out_refs, (rows_ref, acc_ref) = refs[count + 3 : -2], refs[-2:]
    step = pl.program_id(0)
    cap = in_refs[0].shape[0]

    @pl.when(step == 0)
    def _():
        for b, ref in enumerate(in_refs):
            rows_ref[b * cap : (b + 1) * cap, :] = ref[...]

    rows = rows_ref[...]
    gate_proj = jnp.dot(rows, gate_ref[0], preferred_element_type=jnp.float32)
    up_proj = jnp.dot(rows, up_ref[0], preferred_element_type=jnp.float32)
    hidden = (gate_proj / (1.0 + jnp.exp(-gate_proj)) * up_proj).astype(jnp.bfloat16)
    part = jnp.dot(hidden, down_ref[0], preferred_element_type=jnp.float32)

    @pl.when(step == 0)
    def _():
        acc_ref[...] = part

    @pl.when(step > 0)
    def _():
        acc_ref[...] += part

    @pl.when(step == pl.num_programs(0) - 1)
    def _():
        for b, ref in enumerate(out_refs):
            ref[...] = acc_ref[b * cap : (b + 1) * cap, :].astype(ref.dtype)


def expert_blocks(blocks, w_gate, w_up, w_down):
    cap, width = blocks[0].shape
    units = w_gate.shape[2]
    block = math.gcd(units, 512)
    count = len(blocks) * cap
    whole = pl.BlockSpec((cap, width), lambda j: (0, 0))
    return pl.pallas_call(
        functools.partial(expert_body, len(blocks)),
        grid=(units // block,),
        in_specs=[
            *[whole] * len(blocks),
            pl.BlockSpec((1, width, block), lambda j: (0, 0, j)),
            pl.BlockSpec((1, width, block), lambda j: (0, 0, j)),
            pl.BlockSpec((1, block, width), lambda j: (0, j, 0)),
        ],
        out_specs=[whole] * len(blocks),
        out_shape=[jax.ShapeDtypeStruct((cap, width), jnp.bfloat16)] * len(blocks),
        scratch_shapes=[pltpu.VMEM((count, width), jnp.bfloat16), pltpu.VMEM((count, width), jnp.float32)],
        cost_estimate=pl.CostEstimate(
            flops=6 * count * width * units,
            transcendentals=count * units,
            bytes_accessed=6 * width * units + 4 * count * width,
        ),
        compiler_params=pltpu.CompilerParams(
            dimension_semantics=("arbitrary",), vmem_limit_bytes=48 * 2**20
        ),
        name="experts",
    )(*blocks, w_gate, w_up, w_down)


def by_partner(partners):
    half, quarter = partners // 2, partners // 4
    return [range(half, half + quarter), range(half), range(half + quarter, partners)]


def crossed(block, partner):
    return lax.ppermute(block, "sp", [(i, i ^ partner) for i in range(lax.axis_size("sp"))])


def routed_experts(stream, normed, routes, route_weights, gain, w_gate, w_up, w_down, cap):
    partners = lax.axis_size("sp")
    partner = routes ^ lax.axis_index("sp")
    blocks = list(pick_blocks(partner.T, normed, partners, cap))
    groups = by_partner(partners)
    for b in [*groups[0], *groups[2], *groups[1]]:
        if b > 0:
            blocks[b] = crossed(blocks[b], b)
    results = {}
    for group in groups:
        worked = expert_blocks([blocks[b] for b in group], w_gate, w_up, w_down)
        for b, block in zip(group, worked):
            results[b] = crossed(block, b) if b > 0 else block
    rows, width = stream.shape
    early = groups[2][0]
    part = join_call(
        join_body,
        partners,
        0,
        (partner, route_weights),
        [results[b] for b in range(early)],
        jax.ShapeDtypeStruct((rows, width), jnp.float32),
    )
    return join_call(
        last_body,
        partners,
        early,
        (partner, route_weights, gain, stream, part),
        [results[b] for b in groups[2]],
        jax.ShapeDtypeStruct((rows, width), jnp.bfloat16),
    )


def mixer_rows(gate_b, gate_c, value, taps, doc_ids):
    tok_dev, width = gate_b.shape
    tap_reach = TAPS - 1
    ids_bf = jnp.broadcast_to(doc_ids[tok_dev - tap_reach :, None], (tap_reach, 128)).astype(jnp.bfloat16)
    packed = jnp.concatenate([gate_c[tok_dev - tap_reach :], value[tok_dev - tap_reach :], ids_bf], axis=1)
    got = passed_along(packed, "sp", 1).astype(jnp.float32)
    prev_rows = got[:, :width] * got[:, width : 2 * width]
    id_values = doc_ids.astype(jnp.float32)
    ext_ids = jnp.concatenate([got[:, 2 * width], id_values], axis=0)
    product = gate_c.astype(jnp.float32) * value.astype(jnp.float32)
    ext_rows = jnp.concatenate([prev_rows, product], axis=0)
    tap_weights = taps.astype(jnp.float32)
    convolved = tap_weights[0] * product
    for distance in range(1, TAPS):
        earlier = ext_rows[tap_reach - distance : tap_reach - distance + tok_dev]
        same_doc = ext_ids[tap_reach - distance : tap_reach - distance + tok_dev] == id_values
        convolved = convolved + jnp.where(same_doc[:, None], tap_weights[distance] * earlier, 0.0)
    return (gate_b.astype(jnp.float32) * convolved).astype(jnp.bfloat16)


def by_partners(lanes, experts):
    return lanes == 1 and experts >= 4 and experts & (experts - 1) == 0


def per_device(
    resid,
    gate_b,
    gate_c,
    value,
    taps,
    doc_ids,
    out_weight,
    norm_gains,
    routes,
    route_weights,
    w_gate,
    w_up,
    w_down,
):
    rows_blk = resid.shape[0]
    width = resid.shape[1]
    experts = lax.axis_size("sp")
    capacity = max(2, 3 * TOP * rows_blk // (2 * experts))
    offset = lax.axis_index("tp") * rows_blk
    my_routes = lax.dynamic_slice_in_dim(routes, offset, rows_blk, 0)
    my_weights = lax.dynamic_slice_in_dim(route_weights, offset, rows_blk, 0)

    mixed = mixer_rows(gate_b, gate_c, value, taps, doc_ids)
    projected = lax.psum_scatter(
        jnp.dot(mixed, out_weight, preferred_element_type=jnp.float32).astype(jnp.bfloat16),
        "tp",
        scatter_dimension=0,
        tiled=True,
    ).astype(jnp.float32)
    stream = resid.astype(jnp.float32) + rms_scale(projected, norm_gains[0])
    normed = rms_scale(stream, norm_gains[1]).astype(jnp.bfloat16)

    if by_partners(lax.axis_size("tp"), experts):
        return routed_experts(
            stream, normed, my_routes, my_weights, norm_gains[2:3], w_gate, w_up, w_down, capacity
        )

    tables = route_tables(my_routes, my_weights, experts)
    edges = [capacity * c // CHUNKS for c in range(CHUNKS + 1)]
    chunks = [chunk_tables(tables, experts, a, b - a) for a, b in zip(edges, edges[1:])]
    combined = 0.0
    for (onehot, w_high, w_low), first, last in zip(chunks, edges, edges[1:]):
        size = last - first
        outgoing = dot_f32(onehot, normed, ((0,), (0,))).astype(jnp.bfloat16)
        arrived = lax.all_to_all(outgoing.reshape(experts, size, width), "sp", split_axis=0, concat_axis=0, tiled=True)
        rows = lax.all_gather(arrived[None], "tp", axis=0, tiled=True).reshape(-1, width)
        worked = expert_block(rows, w_gate, w_up, w_down)
        result = lax.psum_scatter(worked, "tp", scatter_dimension=0, tiled=True).reshape(experts, size, width)
        returned = lax.all_to_all(result, "sp", split_axis=0, concat_axis=0, tiled=True).reshape(-1, width)
        combined = combined + dot_f32(w_high, returned, ((1,), (0,))) + dot_f32(w_low, returned, ((1,), (0,)))
    return (stream + rms_scale(combined, norm_gains[2])).astype(jnp.bfloat16)


def solution(mesh):
    return jax.shard_map(
        per_device,
        mesh=mesh,
        in_specs=(
            P(("grp", "sp", "tp"), None),
            P(("grp", "sp"), "tp"),
            P(("grp", "sp"), "tp"),
            P(("grp", "sp"), "tp"),
            P(None, "tp"),
            P(("grp", "sp")),
            P("tp", None),
            P(),
            P(("grp", "sp"), None),
            P(("grp", "sp"), None),
            P("sp", None, "tp"),
            P("sp", None, "tp"),
            P("sp", "tp", None),
        ),
        out_specs=P(("grp", "sp", "tp"), None),
        check_vma=False,
    )
```

```python
import functools
import math

import jax
import jax.numpy as jnp
from jax import lax
from jax.experimental import pallas as pl
from jax.experimental.pallas import tpu as pltpu
from jax.sharding import PartitionSpec as P


TAPS = 3
TOP = 2
CHUNKS = 2
EXPERTS_VMEM = 48 * 2**20
SMALL_VMEM = 24 * 2**20

norm_eps = 1e-06


def passed_along(block, axis, distance):
    devices = range(lax.axis_size(axis))
    route = [(i - distance, i) for i in devices if i - distance in devices]
    return lax.ppermute(block, axis, route)


def rms_scale(values, gain_row):
    mean_sq = jnp.mean(values * values, axis=-1, keepdims=True)
    return values * lax.rsqrt(mean_sq + norm_eps) * gain_row


def dot_f32(a, b, dims):
    return lax.dot_general(a, b, (dims, ((), ())), preferred_element_type=jnp.float32)


def route_tables(my_routes, my_weights, experts):
    rows = my_routes.shape[0]
    expert_ids = lax.broadcasted_iota(jnp.int32, (rows, experts), 1)
    shares = my_weights / jnp.sum(my_weights, axis=1, keepdims=True)
    named = jnp.zeros((rows, experts), jnp.bool_)
    share_of = jnp.zeros((rows, experts), jnp.float32)
    for k in range(TOP):
        hit = my_routes[:, k : k + 1] == expert_ids
        named = named | hit
        share_of = share_of + jnp.where(hit, shares[:, k : k + 1], 0.0)
    earlier = (
        lax.broadcasted_iota(jnp.int32, (rows, rows), 0)
        > lax.broadcasted_iota(jnp.int32, (rows, rows), 1)
    ).astype(jnp.bfloat16)
    before = dot_f32(earlier, named.astype(jnp.bfloat16), ((1,), (0,)))
    slot_of = jnp.where(named, before, -1.0).astype(jnp.bfloat16)
    high = lax.reduce_precision(share_of, 8, 7)
    return slot_of, high.astype(jnp.bfloat16), (share_of - high).astype(jnp.bfloat16)


def chunk_tables(tables, experts, first, size):
    slot_of, high, low = tables
    cols = lax.broadcasted_iota(jnp.int32, (experts, experts * size), 1)
    owner = lax.broadcasted_iota(jnp.int32, (experts, experts * size), 0)
    spread = (cols // size == owner).astype(jnp.bfloat16)
    col_slot = (lax.broadcasted_iota(jnp.int32, (1, experts * size), 1) % size + first).astype(jnp.float32)
    taken = dot_f32(slot_of, spread, ((1,), (0,))) == col_slot
    onehot = taken.astype(jnp.bfloat16)
    w_high = jnp.where(taken, dot_f32(high, spread, ((1,), (0,))), 0.0).astype(jnp.bfloat16)
    w_low = jnp.where(taken, dot_f32(low, spread, ((1,), (0,))), 0.0).astype(jnp.bfloat16)
    return onehot, w_high, w_low


def expert_block(rows, w_gate, w_up, w_down):
    return expert_blocks([rows], w_gate, w_up, w_down)[0]


def earlier_than(rows, axis):
    i = lax.broadcasted_iota(jnp.int32, (rows, rows), axis)
    j = lax.broadcasted_iota(jnp.int32, (rows, rows), 1 - axis)
    return jnp.where(i < j, 1.0, 0.0).astype(jnp.bfloat16)


def head_body(
    partners, cap, tail_ref, gate_b_ref, gate_c_ref, value_ref, taps_ref, ids_ref, out_weight_ref, resid_ref,
    gains_ref, routes_ref, stream_ref, *refs,
):
    block_refs = refs[:partners]
    rows_ref, ids_ext_ref, mixed_ref, proj_ref, weight_ref, picked_ref, weight_sem, block_sems = refs[partners:]
    weight_copy = pltpu.make_async_copy(out_weight_ref, weight_ref, weight_sem)
    weight_copy.start()
    rows, width = gate_b_ref.shape
    reach = TAPS - 1
    base = rows_ref.shape[0] - rows

    ids_ext_ref[base:, :] = jnp.broadcast_to(ids_ref[...], (rows, ids_ext_ref.shape[1]))
    ids_ext_ref[base - reach : base, :] = tail_ref[:, 2 * width :].astype(jnp.float32)
    same = [ids_ref[...] == ids_ext_ref[base - k : base - k + rows, 0:1] for k in range(1, TAPS)]
    step = math.gcd(width, 256)

    def mix(j, carry):
        at = pl.multiple_of(j * step, step)
        cols = pl.ds(at, step)
        tail_gate = tail_ref[:, cols].astype(jnp.float32)
        tail_value = tail_ref[:, pl.ds(pl.multiple_of(width + at, step), step)].astype(jnp.float32)
        product = gate_c_ref[:, cols].astype(jnp.float32) * value_ref[:, cols].astype(jnp.float32)
        rows_ref[base - reach : base, :] = tail_gate * tail_value
        rows_ref[base:, :] = product
        taps = taps_ref[:, cols].astype(jnp.float32)
        convolved = taps[0:1] * product
        for k in range(1, TAPS):
            earlier = rows_ref[base - k : base - k + rows, :]
            convolved = convolved + jnp.where(same[k - 1], taps[k : k + 1] * earlier, 0.0)
        mixed_ref[:, cols] = (gate_b_ref[:, cols].astype(jnp.float32) * convolved).astype(jnp.bfloat16)
        return carry

    lax.fori_loop(0, width // step, mix, 0)
    weight_copy.wait()
    proj_ref[...] = jnp.dot(mixed_ref[...], weight_ref[...], preferred_element_type=jnp.float32).astype(jnp.bfloat16)

    lines = math.gcd(rows, 32)

    def normalize(j, carry):
        at = pl.ds(pl.multiple_of(j * lines, lines), lines)
        projected = proj_ref[at, :].astype(jnp.float32)
        stream = resid_ref[at, :].astype(jnp.float32) + rms_scale(projected, gains_ref[0:1, :])
        stream_ref[at, :] = stream
        mixed_ref[at, :] = rms_scale(stream, gains_ref[1:2, :]).astype(jnp.bfloat16)
        return carry

    lax.fori_loop(0, rows // lines, normalize, 0)

    ids = lax.broadcasted_iota(jnp.int32, (partners, rows), 0)
    named = jnp.zeros((partners, rows), jnp.float32)
    for k in range(TOP):
        named = named + jnp.where(routes_ref[k : k + 1, :] == ids, 1.0, 0.0)
    before = dot_f32(named.astype(jnp.bfloat16), earlier_than(rows, 0), ((1,), (0,)))
    slot_of = jnp.where(named > 0.0, before, -1.0).astype(jnp.bfloat16)
    group = math.gcd(partners, 4)
    normed = mixed_ref[...]
    copies = []
    for first in [*range(partners // 2, partners, group), *range(0, partners // 2, group)]:
        line = lax.broadcasted_iota(jnp.int32, (group * cap, partners), 0)
        start = (lax.broadcasted_iota(jnp.int32, (group * cap, partners), 1) - first) * cap
        mine = (line >= start) & (line < start + cap)
        slot = jnp.sum(jnp.where(mine, (line - start).astype(jnp.float32), 0.0), axis=1, keepdims=True)
        spread = jnp.where(mine, 1.0, 0.0).astype(jnp.bfloat16)
        taken = dot_f32(spread, slot_of, ((1,), (0,))) == slot
        onehot = jnp.where(taken, 1.0, 0.0).astype(jnp.bfloat16)
        picked_ref[first * cap : (first + group) * cap, :] = dot_f32(onehot, normed, ((1,), (0,))).astype(
            jnp.bfloat16
        )
        for b in range(first, first + group):
            copies.append(
                pltpu.make_async_copy(picked_ref.at[b * cap : (b + 1) * cap, :], block_refs[b], block_sems.at[b])
            )
            copies[-1].start()
    for copy in copies:
        copy.wait()


def head_call(tail, gate_b, gate_c, value, taps, doc_ids, out_weight, resid, gains, routes_t, partners, cap):
    rows, width = gate_b.shape
    here = pl.BlockSpec(memory_space=pltpu.VMEM)
    far = pl.BlockSpec(memory_space=pltpu.HBM)
    base = 8
    return pl.pallas_call(
        functools.partial(head_body, partners, cap),
        in_specs=[here] * 6 + [far] + [here] * 3,
        out_specs=[here] + [far] * partners,
        out_shape=[
            jax.ShapeDtypeStruct((rows, width), jnp.float32),
            *[jax.ShapeDtypeStruct((cap, width), jnp.bfloat16)] * partners,
        ],
        scratch_shapes=[
            pltpu.VMEM((base + rows, math.gcd(width, 256)), jnp.float32),
            pltpu.VMEM((base + rows, 128), jnp.float32),
            pltpu.VMEM((rows, width), jnp.bfloat16),
            pltpu.VMEM((rows, width), jnp.bfloat16),
            pltpu.VMEM((width, width), jnp.bfloat16),
            pltpu.VMEM((partners * cap, width), jnp.bfloat16),
            pltpu.SemaphoreType.DMA,
            pltpu.SemaphoreType.DMA((partners,)),
        ],
        compiler_params=pltpu.CompilerParams(vmem_limit_bytes=EXPERTS_VMEM),
        name="head",
    )(tail, gate_b, gate_c, value, taps, doc_ids[:, None].astype(jnp.float32), out_weight, resid, gains, routes_t)


def share_columns(partner, share, partners, first, count, cap):
    rows = partner.shape[0]
    ids = lax.broadcasted_iota(jnp.int32, (rows, partners), 1)
    total = share[:, 0:1]
    for k in range(1, TOP):
        total = total + share[:, k : k + 1]
    named = jnp.zeros((rows, partners), jnp.float32)
    share_of = jnp.zeros((rows, partners), jnp.float32)
    for k in range(TOP):
        hit = partner[:, k : k + 1] == ids
        named = named + jnp.where(hit, 1.0, 0.0)
        share_of = share_of + jnp.where(hit, share[:, k : k + 1] / total, 0.0)
    before = dot_f32(earlier_than(rows, 1), named.astype(jnp.bfloat16), ((1,), (0,)))
    slot_of = jnp.where(named > 0.0, before, -1.0).astype(jnp.bfloat16)
    high = share_of.astype(jnp.bfloat16)
    low = (share_of - high.astype(jnp.float32)).astype(jnp.bfloat16)
    cols = lax.broadcasted_iota(jnp.int32, (partners, count * cap), 1)
    start = (lax.broadcasted_iota(jnp.int32, (partners, count * cap), 0) - first) * cap
    mine = (cols >= start) & (cols < start + cap)
    slot = jnp.sum(jnp.where(mine, (cols - start).astype(jnp.float32), 0.0), axis=0, keepdims=True)
    spread = jnp.where(mine, 1.0, 0.0).astype(jnp.bfloat16)
    taken = dot_f32(slot_of, spread, ((1,), (0,))) == slot
    return [
        jnp.where(taken, dot_f32(part, spread, ((1,), (0,))), 0.0).astype(jnp.bfloat16) for part in (high, low)
    ]


def weighted_sum(partners, first, partner_ref, share_ref, block_refs, rows_ref):
    cap = block_refs[0].shape[0]
    for b, ref in enumerate(block_refs):
        rows_ref[b * cap : (b + 1) * cap, :] = ref[...]
    high, low = share_columns(partner_ref[...], share_ref[...], partners, first, len(block_refs), cap)
    rows = rows_ref[...]
    return dot_f32(high, rows, ((1,), (0,))) + dot_f32(low, rows, ((1,), (0,)))


def join_body(partners, first, partner_ref, share_ref, *refs):
    *block_refs, out_ref, rows_ref = refs
    out_ref[...] = weighted_sum(partners, first, partner_ref, share_ref, block_refs, rows_ref)


def last_body(partners, first, partner_ref, share_ref, gain_ref, stream_ref, part_ref, *refs):
    *block_refs, out_ref, rows_ref = refs
    combined = part_ref[...] + weighted_sum(partners, first, partner_ref, share_ref, block_refs, rows_ref)
    out_ref[...] = (stream_ref[...] + rms_scale(combined, gain_ref[...])).astype(out_ref.dtype)


def join_call(body, partners, first, given, blocks, out):
    cap, width = blocks[0].shape
    return pl.pallas_call(
        functools.partial(body, partners, first),
        out_shape=out,
        scratch_shapes=[pltpu.VMEM((len(blocks) * cap, width), jnp.bfloat16)],
        compiler_params=pltpu.CompilerParams(vmem_limit_bytes=SMALL_VMEM),
    )(*given, *blocks)


def expert_body(count, *refs):
    in_refs, (gate_ref, up_ref, down_ref) = refs[:count], refs[count : count + 3]
    out_refs, (rows_ref, acc_ref) = refs[count + 3 : -2], refs[-2:]
    step = pl.program_id(0)
    cap = in_refs[0].shape[0]

    @pl.when(step == 0)
    def _():
        for b, ref in enumerate(in_refs):
            rows_ref[b * cap : (b + 1) * cap, :] = ref[...]

    rows = rows_ref[...]
    gate_proj = jnp.dot(rows, gate_ref[0], preferred_element_type=jnp.float32)
    up_proj = jnp.dot(rows, up_ref[0], preferred_element_type=jnp.float32)
    hidden = (gate_proj / (1.0 + jnp.exp(-gate_proj)) * up_proj).astype(jnp.bfloat16)
    part = jnp.dot(hidden, down_ref[0], preferred_element_type=jnp.float32)

    @pl.when(step == 0)
    def _():
        acc_ref[...] = part

    @pl.when(step > 0)
    def _():
        acc_ref[...] += part

    @pl.when(step == pl.num_programs(0) - 1)
    def _():
        for b, ref in enumerate(out_refs):
            ref[...] = acc_ref[b * cap : (b + 1) * cap, :].astype(ref.dtype)


def expert_blocks(blocks, w_gate, w_up, w_down):
    cap, width = blocks[0].shape
    units = w_gate.shape[2]
    block = math.gcd(units, 512)
    count = len(blocks) * cap
    whole = pl.BlockSpec((cap, width), lambda j: (0, 0))
    return pl.pallas_call(
        functools.partial(expert_body, len(blocks)),
        grid=(units // block,),
        in_specs=[
            *[whole] * len(blocks),
            pl.BlockSpec((1, width, block), lambda j: (0, 0, j)),
            pl.BlockSpec((1, width, block), lambda j: (0, 0, j)),
            pl.BlockSpec((1, block, width), lambda j: (0, j, 0)),
        ],
        out_specs=[whole] * len(blocks),
        out_shape=[jax.ShapeDtypeStruct((cap, width), jnp.bfloat16)] * len(blocks),
        scratch_shapes=[pltpu.VMEM((count, width), jnp.bfloat16), pltpu.VMEM((count, width), jnp.float32)],
        cost_estimate=pl.CostEstimate(
            flops=6 * count * width * units,
            transcendentals=count * units,
            bytes_accessed=6 * width * units + 4 * count * width,
        ),
        compiler_params=pltpu.CompilerParams(
            dimension_semantics=("arbitrary",), vmem_limit_bytes=EXPERTS_VMEM
        ),
        name="experts",
    )(*blocks, w_gate, w_up, w_down)


def by_partner(partners):
    half, quarter = partners // 2, partners // 4
    return [range(half, half + quarter), range(half), range(half + quarter, partners)]


def crossed(block, partner):
    return lax.ppermute(block, "sp", [(i, i ^ partner) for i in range(lax.axis_size("sp"))])


def layer_by_partners(
    resid, gate_b, gate_c, value, taps, doc_ids, out_weight, gains, routes, route_weights, w_gate, w_up, w_down, cap
):
    partners = lax.axis_size("sp")
    partner = routes ^ lax.axis_index("sp")
    tail = tail_passed(gate_c, value, doc_ids)
    stream, *blocks = head_call(
        tail, gate_b, gate_c, value, taps, doc_ids, out_weight, resid, gains, partner.T, partners, cap
    )
    groups = by_partner(partners)
    for b in [*groups[0], *groups[2], *groups[1]]:
        if b > 0:
            blocks[b] = crossed(blocks[b], b)
    results = {}
    for group in groups:
        worked = expert_blocks([blocks[b] for b in group], w_gate, w_up, w_down)
        for b, block in zip(group, worked):
            results[b] = crossed(block, b) if b > 0 else block
    rows, width = stream.shape
    early = groups[2][0]
    part = join_call(
        join_body,
        partners,
        0,
        (partner, route_weights),
        [results[b] for b in range(early)],
        jax.ShapeDtypeStruct((rows, width), jnp.float32),
    )
    return join_call(
        last_body,
        partners,
        early,
        (partner, route_weights, gains[2:3], stream, part),
        [results[b] for b in groups[2]],
        jax.ShapeDtypeStruct((rows, width), jnp.bfloat16),
    )


def tail_passed(gate_c, value, doc_ids):
    tok_dev = gate_c.shape[0]
    tap_reach = TAPS - 1
    ids_bf = jnp.broadcast_to(doc_ids[tok_dev - tap_reach :, None], (tap_reach, 128)).astype(jnp.bfloat16)
    packed = jnp.concatenate([gate_c[tok_dev - tap_reach :], value[tok_dev - tap_reach :], ids_bf], axis=1)
    return passed_along(packed, "sp", 1)


def mixer_rows(gate_b, gate_c, value, taps, doc_ids):
    tok_dev, width = gate_b.shape
    tap_reach = TAPS - 1
    got = tail_passed(gate_c, value, doc_ids).astype(jnp.float32)
    prev_rows = got[:, :width] * got[:, width : 2 * width]
    id_values = doc_ids.astype(jnp.float32)
    ext_ids = jnp.concatenate([got[:, 2 * width], id_values], axis=0)
    product = gate_c.astype(jnp.float32) * value.astype(jnp.float32)
    ext_rows = jnp.concatenate([prev_rows, product], axis=0)
    tap_weights = taps.astype(jnp.float32)
    convolved = tap_weights[0] * product
    for distance in range(1, TAPS):
        earlier = ext_rows[tap_reach - distance : tap_reach - distance + tok_dev]
        same_doc = ext_ids[tap_reach - distance : tap_reach - distance + tok_dev] == id_values
        convolved = convolved + jnp.where(same_doc[:, None], tap_weights[distance] * earlier, 0.0)
    return (gate_b.astype(jnp.float32) * convolved).astype(jnp.bfloat16)


def by_partners(lanes, experts):
    return lanes == 1 and experts >= 4 and experts & (experts - 1) == 0


def per_device(
    resid,
    gate_b,
    gate_c,
    value,
    taps,
    doc_ids,
    out_weight,
    norm_gains,
    routes,
    route_weights,
    w_gate,
    w_up,
    w_down,
):
    rows_blk = resid.shape[0]
    width = resid.shape[1]
    experts = lax.axis_size("sp")
    capacity = max(2, 3 * TOP * rows_blk // (2 * experts))
    if by_partners(lax.axis_size("tp"), experts):
        return layer_by_partners(
            resid, gate_b, gate_c, value, taps, doc_ids, out_weight, norm_gains, routes, route_weights,
            w_gate, w_up, w_down, capacity,
        )

    offset = lax.axis_index("tp") * rows_blk
    my_routes = lax.dynamic_slice_in_dim(routes, offset, rows_blk, 0)
    my_weights = lax.dynamic_slice_in_dim(route_weights, offset, rows_blk, 0)

    mixed = mixer_rows(gate_b, gate_c, value, taps, doc_ids)
    projected = lax.psum_scatter(
        jnp.dot(mixed, out_weight, preferred_element_type=jnp.float32).astype(jnp.bfloat16),
        "tp",
        scatter_dimension=0,
        tiled=True,
    ).astype(jnp.float32)
    stream = resid.astype(jnp.float32) + rms_scale(projected, norm_gains[0])
    normed = rms_scale(stream, norm_gains[1]).astype(jnp.bfloat16)

    tables = route_tables(my_routes, my_weights, experts)
    edges = [capacity * c // CHUNKS for c in range(CHUNKS + 1)]
    chunks = [chunk_tables(tables, experts, a, b - a) for a, b in zip(edges, edges[1:])]
    combined = 0.0
    for (onehot, w_high, w_low), first, last in zip(chunks, edges, edges[1:]):
        size = last - first
        outgoing = dot_f32(onehot, normed, ((0,), (0,))).astype(jnp.bfloat16)
        arrived = lax.all_to_all(outgoing.reshape(experts, size, width), "sp", split_axis=0, concat_axis=0, tiled=True)
        rows = lax.all_gather(arrived[None], "tp", axis=0, tiled=True).reshape(-1, width)
        worked = expert_block(rows, w_gate, w_up, w_down)
        result = lax.psum_scatter(worked, "tp", scatter_dimension=0, tiled=True).reshape(experts, size, width)
        returned = lax.all_to_all(result, "sp", split_axis=0, concat_axis=0, tiled=True).reshape(-1, width)
        combined = combined + dot_f32(w_high, returned, ((1,), (0,))) + dot_f32(w_low, returned, ((1,), (0,)))
    return (stream + rms_scale(combined, norm_gains[2])).astype(jnp.bfloat16)


def solution(mesh):
    return jax.shard_map(
        per_device,
        mesh=mesh,
        in_specs=(
            P(("grp", "sp", "tp"), None),
            P(("grp", "sp"), "tp"),
            P(("grp", "sp"), "tp"),
            P(("grp", "sp"), "tp"),
            P(None, "tp"),
            P(("grp", "sp")),
            P("tp", None),
            P(),
            P(("grp", "sp"), None),
            P(("grp", "sp"), None),
            P("sp", None, "tp"),
            P("sp", None, "tp"),
            P("sp", "tp", None),
        ),
        out_specs=P(("grp", "sp", "tp"), None),
        check_vma=False,
    )
```

```python
import functools
import math

import jax
import jax.numpy as jnp
from jax import lax
from jax.experimental import pallas as pl
from jax.experimental.pallas import tpu as pltpu
from jax.sharding import PartitionSpec as P


TAPS = 3
TOP = 2
CHUNKS = 2
EXPERTS_VMEM = 48 * 2**20
SMALL_VMEM = 24 * 2**20

norm_eps = 1e-06


def passed_along(block, axis, distance):
    devices = range(lax.axis_size(axis))
    route = [(i - distance, i) for i in devices if i - distance in devices]
    return lax.ppermute(block, axis, route)


def rms_scale(values, gain_row):
    mean_sq = jnp.mean(values * values, axis=-1, keepdims=True)
    return values * lax.rsqrt(mean_sq + norm_eps) * gain_row


def dot_f32(a, b, dims):
    return lax.dot_general(a, b, (dims, ((), ())), preferred_element_type=jnp.float32)


def route_tables(my_routes, my_weights, experts):
    rows = my_routes.shape[0]
    expert_ids = lax.broadcasted_iota(jnp.int32, (rows, experts), 1)
    shares = my_weights / jnp.sum(my_weights, axis=1, keepdims=True)
    named = jnp.zeros((rows, experts), jnp.bool_)
    share_of = jnp.zeros((rows, experts), jnp.float32)
    for k in range(TOP):
        hit = my_routes[:, k : k + 1] == expert_ids
        named = named | hit
        share_of = share_of + jnp.where(hit, shares[:, k : k + 1], 0.0)
    earlier = (
        lax.broadcasted_iota(jnp.int32, (rows, rows), 0)
        > lax.broadcasted_iota(jnp.int32, (rows, rows), 1)
    ).astype(jnp.bfloat16)
    before = dot_f32(earlier, named.astype(jnp.bfloat16), ((1,), (0,)))
    slot_of = jnp.where(named, before, -1.0).astype(jnp.bfloat16)
    high = lax.reduce_precision(share_of, 8, 7)
    return slot_of, high.astype(jnp.bfloat16), (share_of - high).astype(jnp.bfloat16)


def chunk_tables(tables, experts, first, size):
    slot_of, high, low = tables
    cols = lax.broadcasted_iota(jnp.int32, (experts, experts * size), 1)
    owner = lax.broadcasted_iota(jnp.int32, (experts, experts * size), 0)
    spread = (cols // size == owner).astype(jnp.bfloat16)
    col_slot = (lax.broadcasted_iota(jnp.int32, (1, experts * size), 1) % size + first).astype(jnp.float32)
    taken = dot_f32(slot_of, spread, ((1,), (0,))) == col_slot
    onehot = taken.astype(jnp.bfloat16)
    w_high = jnp.where(taken, dot_f32(high, spread, ((1,), (0,))), 0.0).astype(jnp.bfloat16)
    w_low = jnp.where(taken, dot_f32(low, spread, ((1,), (0,))), 0.0).astype(jnp.bfloat16)
    return onehot, w_high, w_low


def expert_block(rows, w_gate, w_up, w_down):
    return expert_blocks([rows], w_gate, w_up, w_down)[0]


def earlier_than(rows, axis):
    i = lax.broadcasted_iota(jnp.int32, (rows, rows), axis)
    j = lax.broadcasted_iota(jnp.int32, (rows, rows), 1 - axis)
    return jnp.where(i < j, 1.0, 0.0).astype(jnp.bfloat16)


def pick_body(partners, cap, routes_ref, normed_ref, *refs):
    block_refs, (picked_ref, sems) = refs[:partners], refs[partners:]
    rows = normed_ref.shape[0]
    ids = lax.broadcasted_iota(jnp.int32, (partners, rows), 0)
    named = jnp.zeros((partners, rows), jnp.float32)
    for k in range(TOP):
        named = named + jnp.where(routes_ref[k : k + 1, :] == ids, 1.0, 0.0)
    before = dot_f32(named.astype(jnp.bfloat16), earlier_than(rows, 0), ((1,), (0,)))
    slot_of = jnp.where(named > 0.0, before, -1.0).astype(jnp.bfloat16)
    group = math.gcd(partners, 4)
    normed = normed_ref[...]
    copies = []
    for first in range(0, partners, group):
        line = lax.broadcasted_iota(jnp.int32, (group * cap, partners), 0)
        start = (lax.broadcasted_iota(jnp.int32, (group * cap, partners), 1) - first) * cap
        mine = (line >= start) & (line < start + cap)
        slot = jnp.sum(jnp.where(mine, (line - start).astype(jnp.float32), 0.0), axis=1, keepdims=True)
        spread = jnp.where(mine, 1.0, 0.0).astype(jnp.bfloat16)
        taken = dot_f32(spread, slot_of, ((1,), (0,))) == slot
        onehot = jnp.where(taken, 1.0, 0.0).astype(jnp.bfloat16)
        picked = dot_f32(onehot, normed, ((1,), (0,))).astype(jnp.bfloat16)
        picked_ref[first * cap : (first + group) * cap, :] = picked
        for b in range(first, first + group):
            copies.append(
                pltpu.make_async_copy(picked_ref.at[b * cap : (b + 1) * cap, :], block_refs[b], sems.at[b])
            )
            copies[-1].start()
    for copy in copies:
        copy.wait()


def pick_blocks(partner_t, normed, partners, cap):
    width = normed.shape[1]
    return pl.pallas_call(
        functools.partial(pick_body, partners, cap),
        out_specs=[pl.BlockSpec(memory_space=pltpu.HBM)] * partners,
        out_shape=[pltpu.HBM((cap, width), jnp.bfloat16)] * partners,
        scratch_shapes=[pltpu.VMEM((partners * cap, width), jnp.bfloat16), pltpu.SemaphoreType.DMA((partners,))],
        compiler_params=pltpu.CompilerParams(vmem_limit_bytes=SMALL_VMEM),
        name="pick",
    )(partner_t, normed)


def share_columns(partner, share, partners, first, count, cap):
    rows = partner.shape[0]
    ids = lax.broadcasted_iota(jnp.int32, (rows, partners), 1)
    total = share[:, 0:1]
    for k in range(1, TOP):
        total = total + share[:, k : k + 1]
    named = jnp.zeros((rows, partners), jnp.float32)
    share_of = jnp.zeros((rows, partners), jnp.float32)
    for k in range(TOP):
        hit = partner[:, k : k + 1] == ids
        named = named + jnp.where(hit, 1.0, 0.0)
        share_of = share_of + jnp.where(hit, share[:, k : k + 1] / total, 0.0)
    before = dot_f32(earlier_than(rows, 1), named.astype(jnp.bfloat16), ((1,), (0,)))
    slot_of = jnp.where(named > 0.0, before, -1.0).astype(jnp.bfloat16)
    high = share_of.astype(jnp.bfloat16)
    low = (share_of - high.astype(jnp.float32)).astype(jnp.bfloat16)
    cols = lax.broadcasted_iota(jnp.int32, (partners, count * cap), 1)
    start = (lax.broadcasted_iota(jnp.int32, (partners, count * cap), 0) - first) * cap
    mine = (cols >= start) & (cols < start + cap)
    slot = jnp.sum(jnp.where(mine, (cols - start).astype(jnp.float32), 0.0), axis=0, keepdims=True)
    spread = jnp.where(mine, 1.0, 0.0).astype(jnp.bfloat16)
    taken = dot_f32(slot_of, spread, ((1,), (0,))) == slot
    return [
        jnp.where(taken, dot_f32(part, spread, ((1,), (0,))), 0.0).astype(jnp.bfloat16) for part in (high, low)
    ]


def weighted_sum(partners, first, partner_ref, share_ref, block_refs, rows_ref):
    cap = block_refs[0].shape[0]
    for b, ref in enumerate(block_refs):
        rows_ref[b * cap : (b + 1) * cap, :] = ref[...]
    high, low = share_columns(partner_ref[...], share_ref[...], partners, first, len(block_refs), cap)
    rows = rows_ref[...]
    return dot_f32(high, rows, ((1,), (0,))) + dot_f32(low, rows, ((1,), (0,)))


def join_body(partners, first, partner_ref, share_ref, *refs):
    *block_refs, out_ref, rows_ref = refs
    out_ref[...] = weighted_sum(partners, first, partner_ref, share_ref, block_refs, rows_ref)


def last_body(partners, first, partner_ref, share_ref, gain_ref, stream_ref, part_ref, *refs):
    *block_refs, out_ref, rows_ref = refs
    combined = part_ref[...] + weighted_sum(partners, first, partner_ref, share_ref, block_refs, rows_ref)
    out_ref[...] = (stream_ref[...] + rms_scale(combined, gain_ref[...])).astype(out_ref.dtype)


def join_call(body, partners, first, given, blocks, out):
    cap, width = blocks[0].shape
    return pl.pallas_call(
        functools.partial(body, partners, first),
        out_shape=out,
        scratch_shapes=[pltpu.VMEM((len(blocks) * cap, width), jnp.bfloat16)],
        compiler_params=pltpu.CompilerParams(vmem_limit_bytes=SMALL_VMEM),
    )(*given, *blocks)


def expert_body(count, *refs):
    in_refs, (gate_ref, up_ref, down_ref) = refs[:count], refs[count : count + 3]
    out_refs, (rows_ref, acc_ref) = refs[count + 3 : -2], refs[-2:]
    step = pl.program_id(0)
    cap = in_refs[0].shape[0]

    @pl.when(step == 0)
    def _():
        for b, ref in enumerate(in_refs):
            rows_ref[b * cap : (b + 1) * cap, :] = ref[...]

    rows = rows_ref[...]
    gate_proj = jnp.dot(rows, gate_ref[0], preferred_element_type=jnp.float32)
    up_proj = jnp.dot(rows, up_ref[0], preferred_element_type=jnp.float32)
    hidden = (gate_proj / (1.0 + jnp.exp(-gate_proj)) * up_proj).astype(jnp.bfloat16)
    part = jnp.dot(hidden, down_ref[0], preferred_element_type=jnp.float32)

    @pl.when(step == 0)
    def _():
        acc_ref[...] = part

    @pl.when(step > 0)
    def _():
        acc_ref[...] += part

    @pl.when(step == pl.num_programs(0) - 1)
    def _():
        for b, ref in enumerate(out_refs):
            ref[...] = acc_ref[b * cap : (b + 1) * cap, :].astype(ref.dtype)


def expert_blocks(blocks, w_gate, w_up, w_down):
    cap, width = blocks[0].shape
    units = w_gate.shape[2]
    block = math.gcd(units, 1024)
    count = len(blocks) * cap
    whole = pl.BlockSpec((cap, width), lambda j: (0, 0))
    return pl.pallas_call(
        functools.partial(expert_body, len(blocks)),
        grid=(units // block,),
        in_specs=[
            *[whole] * len(blocks),
            pl.BlockSpec((1, width, block), lambda j: (0, 0, j)),
            pl.BlockSpec((1, width, block), lambda j: (0, 0, j)),
            pl.BlockSpec((1, block, width), lambda j: (0, j, 0)),
        ],
        out_specs=[whole] * len(blocks),
        out_shape=[jax.ShapeDtypeStruct((cap, width), jnp.bfloat16)] * len(blocks),
        scratch_shapes=[pltpu.VMEM((count, width), jnp.bfloat16), pltpu.VMEM((count, width), jnp.float32)],
        cost_estimate=pl.CostEstimate(
            flops=6 * count * width * units,
            transcendentals=count * units,
            bytes_accessed=6 * width * units + 4 * count * width,
        ),
        compiler_params=pltpu.CompilerParams(
            dimension_semantics=("arbitrary",), vmem_limit_bytes=EXPERTS_VMEM
        ),
        name="experts",
    )(*blocks, w_gate, w_up, w_down)


def by_partner(partners):
    half, quarter = partners // 2, partners // 4
    return range(quarter), range(quarter, half), range(half, half + quarter), range(half + quarter, partners)


def crossed(block, partner):
    return lax.ppermute(block, "sp", [(i, i ^ partner) for i in range(lax.axis_size("sp"))])


def routed_experts(stream, normed, routes, route_weights, gain, w_gate, w_up, w_down, cap):
    partners = lax.axis_size("sp")
    partner = routes ^ lax.axis_index("sp")
    blocks = list(pick_blocks(partner.T, normed, partners, cap))
    same, near, far_a, far_b = by_partner(partners)
    for b in range(partners):
        if b > 0:
            blocks[b] = crossed(blocks[b], b)
    results = {}
    for group in [same, far_a, [*near, *far_b]]:
        worked = expert_blocks([blocks[b] for b in group], w_gate, w_up, w_down)
        for b, block in zip(group, worked):
            results[b] = crossed(block, b) if b > 0 else block
    rows, width = stream.shape
    early = far_b[0]
    part = join_call(
        join_body,
        partners,
        0,
        (partner, route_weights),
        [results[b] for b in range(early)],
        jax.ShapeDtypeStruct((rows, width), jnp.float32),
    )
    return join_call(
        last_body,
        partners,
        early,
        (partner, route_weights, gain, stream, part),
        [results[b] for b in far_b],
        jax.ShapeDtypeStruct((rows, width), jnp.bfloat16),
    )


def tail_passed(gate_c, value, doc_ids):
    tok_dev = gate_c.shape[0]
    tap_reach = TAPS - 1
    ids_bf = jnp.broadcast_to(doc_ids[tok_dev - tap_reach :, None], (tap_reach, 128)).astype(jnp.bfloat16)
    packed = jnp.concatenate([gate_c[tok_dev - tap_reach :], value[tok_dev - tap_reach :], ids_bf], axis=1)
    return passed_along(packed, "sp", 1)


def mixer_rows(gate_b, gate_c, value, taps, doc_ids):
    tok_dev, width = gate_b.shape
    tap_reach = TAPS - 1
    got = tail_passed(gate_c, value, doc_ids).astype(jnp.float32)
    prev_rows = got[:, :width] * got[:, width : 2 * width]
    id_values = doc_ids.astype(jnp.float32)
    ext_ids = jnp.concatenate([got[:, 2 * width], id_values], axis=0)
    product = gate_c.astype(jnp.float32) * value.astype(jnp.float32)
    ext_rows = jnp.concatenate([prev_rows, product], axis=0)
    tap_weights = taps.astype(jnp.float32)
    convolved = tap_weights[0] * product
    for distance in range(1, TAPS):
        earlier = ext_rows[tap_reach - distance : tap_reach - distance + tok_dev]
        same_doc = ext_ids[tap_reach - distance : tap_reach - distance + tok_dev] == id_values
        convolved = convolved + jnp.where(same_doc[:, None], tap_weights[distance] * earlier, 0.0)
    return (gate_b.astype(jnp.float32) * convolved).astype(jnp.bfloat16)


def by_partners(lanes, experts):
    return lanes == 1 and experts >= 4 and experts & (experts - 1) == 0


def per_device(
    resid,
    gate_b,
    gate_c,
    value,
    taps,
    doc_ids,
    out_weight,
    norm_gains,
    routes,
    route_weights,
    w_gate,
    w_up,
    w_down,
):
    rows_blk = resid.shape[0]
    width = resid.shape[1]
    experts = lax.axis_size("sp")
    capacity = max(2, 3 * TOP * rows_blk // (2 * experts))
    offset = lax.axis_index("tp") * rows_blk
    my_routes = lax.dynamic_slice_in_dim(routes, offset, rows_blk, 0)
    my_weights = lax.dynamic_slice_in_dim(route_weights, offset, rows_blk, 0)

    mixed = mixer_rows(gate_b, gate_c, value, taps, doc_ids)
    projected = lax.psum_scatter(
        jnp.dot(mixed, out_weight, preferred_element_type=jnp.float32).astype(jnp.bfloat16),
        "tp",
        scatter_dimension=0,
        tiled=True,
    ).astype(jnp.float32)
    stream = resid.astype(jnp.float32) + rms_scale(projected, norm_gains[0])
    normed = rms_scale(stream, norm_gains[1]).astype(jnp.bfloat16)

    if by_partners(lax.axis_size("tp"), experts):
        return routed_experts(
            stream, normed, my_routes, my_weights, norm_gains[2:3], w_gate, w_up, w_down, capacity
        )

    tables = route_tables(my_routes, my_weights, experts)
    edges = [capacity * c // CHUNKS for c in range(CHUNKS + 1)]
    chunks = [chunk_tables(tables, experts, a, b - a) for a, b in zip(edges, edges[1:])]
    combined = 0.0
    for (onehot, w_high, w_low), first, last in zip(chunks, edges, edges[1:]):
        size = last - first
        outgoing = dot_f32(onehot, normed, ((0,), (0,))).astype(jnp.bfloat16)
        arrived = lax.all_to_all(outgoing.reshape(experts, size, width), "sp", split_axis=0, concat_axis=0, tiled=True)
        rows = lax.all_gather(arrived[None], "tp", axis=0, tiled=True).reshape(-1, width)
        worked = expert_block(rows, w_gate, w_up, w_down)
        result = lax.psum_scatter(worked, "tp", scatter_dimension=0, tiled=True).reshape(experts, size, width)
        returned = lax.all_to_all(result, "sp", split_axis=0, concat_axis=0, tiled=True).reshape(-1, width)
        combined = combined + dot_f32(w_high, returned, ((1,), (0,))) + dot_f32(w_low, returned, ((1,), (0,)))
    return (stream + rms_scale(combined, norm_gains[2])).astype(jnp.bfloat16)


def solution(mesh):
    return jax.shard_map(
        per_device,
        mesh=mesh,
        in_specs=(
            P(("grp", "sp", "tp"), None),
            P(("grp", "sp"), "tp"),
            P(("grp", "sp"), "tp"),
            P(("grp", "sp"), "tp"),
            P(None, "tp"),
            P(("grp", "sp")),
            P("tp", None),
            P(),
            P(("grp", "sp"), None),
            P(("grp", "sp"), None),
            P("sp", None, "tp"),
            P("sp", None, "tp"),
            P("sp", "tp", None),
        ),
        out_specs=P(("grp", "sp", "tp"), None),
        check_vma=False,
    )
```
